32 devices in a mesh: ep: 8 (over z, x), tp: 4 (over y, core).
Axes of the slice: x: 2, y: 2, z: 4, core: 2. Of those that a mesh axis runs over, the one named last changes fastest.
Arguments:
- tokens: bfloat16 [256, 2048], P('ep'), may hold values from -24 to 24
- norm_gain: float32 [2048], replicated, may hold values from 0.1 to 1.9
- post_gain: float32 [2048], replicated, may hold values from 0.1 to 1.9
- w_query: bfloat16 [2048, 2048], P(None, 'tp'), may hold values from -0.125 to 0.125
- w_key: bfloat16 [2048, 512], P(None, 'tp'), may hold values from -0.125 to 0.125
- w_value: bfloat16 [2048, 512], P(None, 'tp'), may hold values from -0.125 to 0.125
- w_forget: bfloat16 [2048, 32], replicated, may hold values from -0.25 to 0.25
- w_output: bfloat16 [2048, 2048], P('tp'), may hold values from -0.125 to 0.125
- key_cache: bfloat16 [256, 8, 64, 1024], P('ep', 'tp'), may hold values from -660 to 660
- value_cache: bfloat16 [256, 8, 64, 1024], P('ep', 'tp'), may hold values from -6 to 6
- gate_cache: float32 [256, 32, 1024], P('ep', 'tp'), may hold values from -176.08 to 0, as said below
- lengths: int32 [256], P('ep'), may hold values from 256 to 1024
- routes: int32 [256, 2], P('ep'), may hold values from 0 to 7, all different within a row; in each aligned block of 32 rows (0 to 31, 32 to 63, ...) at most 16 rows name the same one
- route_logits: float32 [256, 2], P('ep'), may hold values from -6 to 6
- w_gate: bfloat16 [8, 2048, 3584], P('ep', None, 'tp'), may hold values from -0.125 to 0.125
- w_up: bfloat16 [8, 2048, 3584], P('ep', None, 'tp'), may hold values from -0.125 to 0.125
- w_down: bfloat16 [8, 3584, 2048], P('ep', 'tp'), may hold values from -0.09375 to 0.09375
Outputs:
- layer_out: bfloat16 [256, 2048], P('ep', 'tp')
The draws below stay inside these ranges and needn't reach their ends.
Inputs may be any that keep to these rules, and one draw needn't show every extreme that they name: `routes`: each row names 2 different experts. The rows of one index of ep name any one expert at most 16 times, and in every draw some index of ep names some expert exactly 16 times. `gate_cache`: cumulative sums of negative log forget gates along positions: nonincreasing along the last dimension. `lengths`: the new token follows the valid positions of its sequence.
All inputs are finite; a program needn't handle non-finite values.
Results may differ from the reference program's by a relative error of at most 0.011.
Values may be sent and summed in bfloat16 or wider, within the bound.
A program may use at most 64 MiB of HBM per device.

```python
import math
import jax
import jax.numpy as jnp
import numpy as np
from jax import lax

WIDTH = 2048
QUERY_HEADS = 32
HEAD_DIM = 64
KV_HEADS = 8
FFN = 3584
TOPK = 2
TOK_GRP = 32
CACHE_POSITIONS = 1024
SEQUENCE_TOTAL = 256
EXPERTS = 8
CAP = 16
N_EP = 8
N_TP = 4


def draw_tokens(key, part):
    first, second = jax.random.split(jax.random.fold_in(key, 3))
    row_scale = jnp.exp(jax.random.uniform(first, (SEQUENCE_TOTAL, 1), jnp.float32, jnp.log(0.3), jnp.log(3.0)))
    column_scale = 0.4 * jnp.exp(jnp.log(4.0) * jnp.arange(WIDTH, dtype=jnp.float32) / WIDTH)
    base = jnp.clip(jax.random.normal(second, (SEQUENCE_TOTAL, WIDTH), jnp.float32), -5.0, 5.0)
    return (row_scale * column_scale[None, :] * base).astype(jnp.bfloat16)


def draw_key_cache(key, part):
    first = jax.random.fold_in(jax.random.fold_in(key, 5), 0)
    base = jnp.clip(jax.random.normal(first, (SEQUENCE_TOTAL, KV_HEADS, HEAD_DIM, CACHE_POSITIONS), jnp.float32), -6.0, 6.0)
    return base.astype(jnp.bfloat16)


def draw_gate_cache(key, part):
    key_entries = jax.random.split(jax.random.fold_in(key, 7), 7)
    slow_share = 0.5
    keeps = jax.random.uniform(key_entries[0], (SEQUENCE_TOTAL, QUERY_HEADS, 1), jnp.float32) < slow_share
    slow_total = jax.random.uniform(key_entries[1], (SEQUENCE_TOTAL, QUERY_HEADS, 1), jnp.float32, 0.2, 0.9)
    fast_rate = jnp.exp(jax.random.uniform(key_entries[2], (SEQUENCE_TOTAL, QUERY_HEADS, 1), jnp.float32, jnp.log(0.03), jnp.log(0.1)))
    decay_rate = jnp.where(keeps, slow_total / CACHE_POSITIONS, fast_rate)
    coarse_estimate = jax.random.uniform(key_entries[3], (SEQUENCE_TOTAL, QUERY_HEADS, CACHE_POSITIONS), jnp.float32, 0.3, 1.7)
    cache_position = jnp.arange(CACHE_POSITIONS, dtype=jnp.int32)[None, None, :]
    leading_group = jax.random.randint(key_entries[4], (SEQUENCE_TOTAL, QUERY_HEADS, 1), 0, CACHE_POSITIONS)
    trailing_group = jax.random.randint(key_entries[5], (SEQUENCE_TOTAL, QUERY_HEADS, 1), 0, CACHE_POSITIONS)
    group_length = jax.random.uniform(key_entries[6], (SEQUENCE_TOTAL, QUERY_HEADS, 2), jnp.float32, 0.22, 0.69)
    position_groups = (cache_position == leading_group).astype(jnp.float32) * group_length[:, :, 0:1] + (cache_position == trailing_group).astype(jnp.float32) * group_length[:, :, 1:2]
    decode_steps = -decay_rate * coarse_estimate - position_groups
    return jnp.cumsum(decode_steps, axis=-1).astype(jnp.float32)


def with_ends(entries, rng, least, high):
    index_at = [jax.random.randint(jax.random.fold_in(rng, axis), (), 0, length) for axis, length in enumerate(entries.shape)]
    widest = entries.shape.index(max(entries.shape))
    beside = index_at[:widest] + [(index_at[widest] + 1) % entries.shape[widest]] + index_at[widest + 1:]
    return entries.at[tuple(index_at)].set(least).at[tuple(beside)].set(high)


def block_levels(stream_key, extent, cuts, low, largest):
    loudness, own = 1.0, jax.random.fold_in(stream_key, 6)
    for position, blocks in cuts:
        draws = jnp.exp(jax.random.uniform(jax.random.fold_in(own, position), (blocks,), jnp.float32, low / len(cuts), largest / len(cuts)))
        loudness = loudness * jnp.repeat(draws, extent[position] // blocks).reshape([-1 if axis == position else 1 for axis in range(len(extent))])
    return loudness


def assign_block(key, own, number, rows, count, top, bound, lean):
    ranking = jax.random.permutation(key, count)
    crowded, ordinary = load_shares(count, rows * top, bound, lean, True), load_shares(count, rows * top, bound, lean, False)
    places = jnp.arange(count)

    def named(sizes, rotation):
        used = int((sizes > 0).sum())
        fixed = max(1, used // 4)
        moved = fixed + (places - fixed + rotation * (used - fixed)) % max(1, count - fixed)
        return jnp.zeros((count,), jnp.int32).at[ranking[jnp.where(places < fixed, places, moved)]].set(jnp.asarray(sizes, jnp.int32))

    sizes = jnp.where(number % 4 == 0, named(crowded, number // 4), named(ordinary, number - number // 4 - 1))
    mixed = jax.random.permutation(jax.random.fold_in(own, 3), count)
    giver, receiver = mixed[0:count // 2 * 2:2], mixed[1:count // 2 * 2:2]
    slack = jnp.minimum(sizes[giver] - 1, bound - sizes[receiver]) // 2
    slack = jnp.where((giver == ranking[0]) | (receiver == ranking[0]) | (sizes[receiver] == 0), 0, jnp.maximum(slack, 0))
    moved = jax.random.randint(jax.random.fold_in(own, 4), (count // 2,), 0, 1 << 20) % (slack + 1)
    sizes = sizes.at[giver].add(-moved).at[receiver].add(moved)
    labels = jnp.searchsorted(jnp.cumsum(sizes), jnp.arange(rows * top), side="right").astype(jnp.int32)
    listing = labels.reshape(top, rows).T
    listing = listing[jax.random.permutation(jax.random.fold_in(own, 1), rows)]
    rotation = jax.random.randint(jax.random.fold_in(own, 2), (rows, 1), 0, top)
    return jnp.take_along_axis(listing, (jnp.arange(top)[None, :] + rotation) % top, axis=1)


def load_shares(count, total, most, lean, full):
    portions = [(1 << 20) // math.isqrt(grade ** lean) + 1 for grade in range(1, count + 1)]
    largest = most if full else min(most, max(-(-total // count), total * portions[0] // sum(portions)))
    least = 1 if total - largest >= count - 1 else 0
    holding, rest = [largest] + [least] * (count - 1), total - largest - least * (count - 1)
    while rest > 0:
        candidates = [i for i in range(1, count) if holding[i] < largest] or [i for i in range(1, count) if holding[i] < most]
        mass, remaining = sum([portions[i] for i in candidates]), rest
        for i in candidates:
            more = min(most - holding[i], max(1, remaining * portions[i] // mass), rest)
            holding[i] = holding[i] + more
            rest = rest - more
    return np.array(holding)


def bell_draw(rng, extent, scale, bound, shards=(), kind=jnp.bfloat16):
    values = jax.random.normal(rng, extent, jnp.float32) * scale
    if len(shards) > 0:
        values = block_levels(rng, extent, shards, -0.22, 0.18) * values
    return jnp.clip(values, min=-bound, max=bound).astype(kind)


def setup_inputs(seed: int = 0) -> dict:
    seeds = jax.random.split(jax.random.key(seed), 18)
    tokens = draw_tokens(jax.random.fold_in(seeds[17], 71), 0)
    norm_gain = jnp.clip(1.0 + 0.18 * jax.random.normal(seeds[1], (WIDTH,), jnp.float32), 0.1, 1.9)
    post_gain = jnp.clip(1.0 + 0.18 * jax.random.normal(seeds[2], (WIDTH,), jnp.float32), 0.1, 1.9)
    w_query = bell_draw(seeds[3], (WIDTH, QUERY_HEADS * HEAD_DIM), WIDTH ** -0.5, 0.125, ((1, 4),))
    w_key = bell_draw(seeds[4], (WIDTH, KV_HEADS * HEAD_DIM), WIDTH ** -0.5, 0.125, ((1, 4),))
    w_value = bell_draw(seeds[5], (WIDTH, KV_HEADS * HEAD_DIM), WIDTH ** -0.5, 0.125, ((1, 4),))
    w_forget = bell_draw(seeds[6], (WIDTH, QUERY_HEADS), (WIDTH // 4) ** -0.5, 0.25)
    w_output = bell_draw(seeds[7], (QUERY_HEADS * HEAD_DIM, WIDTH), (QUERY_HEADS * HEAD_DIM) ** -0.5, 0.125, ((0, 4),))
    key_cache = draw_key_cache(jax.random.fold_in(seeds[17], 71), 0)
    value_cache = bell_draw(seeds[9], (SEQUENCE_TOTAL, KV_HEADS, HEAD_DIM, CACHE_POSITIONS), 1.0, 6.0, ((0, 8), (1, 4)))
    gate_cache = draw_gate_cache(jax.random.fold_in(seeds[17], 71), 0)
    lengths = with_ends(jax.random.randint(seeds[11], (SEQUENCE_TOTAL,), CACHE_POSITIONS // 4, CACHE_POSITIONS + 1), jax.random.fold_in(seeds[11], 1), CACHE_POSITIONS // 4, CACHE_POSITIONS).astype(jnp.int32)
    routes_keys = jax.random.split(jax.random.fold_in(seeds[12], 1), SEQUENCE_TOTAL // TOK_GRP)
    routes_turns = jax.random.permutation(jax.random.fold_in(seeds[12], 3), SEQUENCE_TOTAL // TOK_GRP)
    routes = jax.vmap(lambda own, number: assign_block(jax.random.fold_in(seeds[12], 2), own, number, TOK_GRP, EXPERTS, TOPK, CAP, 2))(routes_keys, routes_turns).reshape((SEQUENCE_TOTAL, TOPK))
    route_logits = bell_draw(seeds[13], (SEQUENCE_TOTAL, TOPK), 1.5, 6.0, ((0, 8),), jnp.float32)
    w_gate = bell_draw(seeds[14], (EXPERTS, WIDTH, FFN), WIDTH ** -0.5, 0.125, ((0, 8), (2, 4)))
    w_up = bell_draw(seeds[15], (EXPERTS, WIDTH, FFN), WIDTH ** -0.5, 0.125, ((0, 8), (2, 4)))
    w_down = bell_draw(seeds[16], (EXPERTS, FFN, WIDTH), FFN ** -0.5, 0.09375, ((0, 8), (1, 4)))
    return dict(tokens=tokens, norm_gain=norm_gain, post_gain=post_gain, w_query=w_query, w_key=w_key, w_value=w_value, w_forget=w_forget, w_output=w_output, key_cache=key_cache, value_cache=value_cache, gate_cache=gate_cache, lengths=lengths, routes=routes, route_logits=route_logits, w_gate=w_gate, w_up=w_up, w_down=w_down)


epsilon = 1e-06

def normalize(rows, gain):
    return rows * lax.rsqrt(lax.optimization_barrier(jnp.mean(rows * rows, axis=-1, keepdims=True)) + epsilon) * gain

def attend_one(packed):
    query_vector, fresh_key, value_new, log_forget, key_rows, value_rows, gates, length = packed
    group_size = QUERY_HEADS // KV_HEADS
    score_scale = HEAD_DIM ** (-0.5)
    grouped = query_vector.reshape(KV_HEADS, group_size, HEAD_DIM).astype(jnp.float32)
    past_scores = jnp.einsum('kgd,kdl->kgl', grouped, key_rows.astype(jnp.float32)).reshape(QUERY_HEADS, CACHE_POSITIONS)
    cache_position = jnp.arange(CACHE_POSITIONS, dtype=jnp.int32)[None, :]
    latest = lax.optimization_barrier(jnp.sum(jnp.where(cache_position == length - 1, gates, 0.0), axis=-1))
    past_scores = past_scores * score_scale + (latest + log_forget)[:, None] - gates
    past_scores = jnp.where(cache_position < length, past_scores, -jnp.inf)
    new_score = jnp.einsum('kgd,kd->kg', grouped, fresh_key.astype(jnp.float32)).reshape(QUERY_HEADS) * score_scale
    peak_score = jnp.maximum(lax.optimization_barrier(jnp.max(past_scores, axis=-1)), new_score)
    past_exp = jnp.exp(past_scores - peak_score[:, None])
    new_exp = jnp.exp(new_score - peak_score)
    denominator = lax.optimization_barrier(jnp.sum(past_exp, axis=-1)) + new_exp
    past_prob = (past_exp / denominator[:, None]).astype(jnp.bfloat16)
    new_prob = (new_exp / denominator).astype(jnp.bfloat16)
    mixed = jnp.einsum('kgl,kdl->kgd', past_prob.reshape(KV_HEADS, group_size, CACHE_POSITIONS).astype(jnp.float32), value_rows.astype(jnp.float32))
    mixed = mixed + new_prob.reshape(KV_HEADS, group_size)[:, :, None].astype(jnp.float32) * value_new[:, None, :].astype(jnp.float32)
    return mixed.reshape(QUERY_HEADS * HEAD_DIM).astype(jnp.bfloat16)

def reference(tokens, norm_gain, post_gain, w_query, w_key, w_value, w_forget, w_output, key_cache, value_cache, gate_cache, lengths, routes, route_logits, w_gate, w_up, w_down):
    tokens_wide = tokens.astype(jnp.float32)
    normed = normalize(tokens_wide, norm_gain).astype(jnp.bfloat16)
    query_vector = jnp.dot(normed, w_query, preferred_element_type=jnp.float32).astype(jnp.bfloat16)
    fresh_key = jnp.dot(normed, w_key, preferred_element_type=jnp.float32).astype(jnp.bfloat16)
    value_new = jnp.dot(normed, w_value, preferred_element_type=jnp.float32).astype(jnp.bfloat16)
    log_forget = jax.nn.log_sigmoid(jnp.dot(normed, w_forget, preferred_element_type=jnp.float32))
    attended = lax.map(attend_one, (query_vector, fresh_key.reshape(SEQUENCE_TOTAL, KV_HEADS, HEAD_DIM), value_new.reshape(SEQUENCE_TOTAL, KV_HEADS, HEAD_DIM), log_forget, key_cache, value_cache, gate_cache, lengths))
    head_block = QUERY_HEADS * HEAD_DIM // N_TP
    blocks = attended.reshape(SEQUENCE_TOTAL, N_TP, head_block).transpose(1, 0, 2).astype(jnp.float32)
    parts = jnp.einsum('tsr,trw->tsw', blocks, w_output.reshape(N_TP, head_block, WIDTH).astype(jnp.float32))
    attention = lax.optimization_barrier(jnp.sum(parts.astype(jnp.bfloat16).astype(jnp.float32), axis=0))
    stream = tokens_wide + attention
    expert_input = normalize(stream, post_gain).astype(jnp.bfloat16)
    route_count = SEQUENCE_TOTAL * TOPK
    per_expert = CAP * N_EP
    flat_routes = routes.reshape(route_count)
    expert_onehot = (flat_routes[:, None] == jnp.arange(EXPERTS, dtype=jnp.int32)[None, :]).astype(jnp.int32)
    route_rank = lax.optimization_barrier(jnp.sum(jnp.cumsum(expert_onehot, axis=0) * expert_onehot, axis=1)) - 1
    slot_index = (flat_routes * per_expert + route_rank).astype(jnp.int32)
    slot_token = jnp.zeros((EXPERTS * per_expert,), jnp.int32).at[slot_index].set(jnp.arange(route_count, dtype=jnp.int32) // TOPK)
    ff_block = FFN // N_TP

    def run_expert(index):
        chosen = lax.dynamic_slice_in_dim(slot_token, (index * per_expert).astype(jnp.int32), per_expert)
        expert_rows = expert_input[chosen]
        gate_act = jnp.dot(expert_rows, w_gate[index], preferred_element_type=jnp.float32)
        upper = jnp.dot(expert_rows, w_up[index], preferred_element_type=jnp.float32)
        hidden_act = (jax.nn.silu(gate_act) * upper).astype(jnp.bfloat16)
        down_parts = jnp.einsum('rtf,tfw->trw', hidden_act.reshape(per_expert, N_TP, ff_block).astype(jnp.float32), w_down[index].reshape(N_TP, ff_block, WIDTH).astype(jnp.float32))
        return lax.optimization_barrier(jnp.sum(down_parts.astype(jnp.bfloat16).astype(jnp.float32), axis=0)).astype(jnp.bfloat16)
    outputs = lax.map(run_expert, jnp.arange(EXPERTS, dtype=jnp.int32))
    picked = outputs.reshape(EXPERTS * per_expert, WIDTH)[slot_index].astype(jnp.float32).reshape(SEQUENCE_TOTAL, TOPK, WIDTH)
    route_weight = jax.nn.softmax(route_logits, axis=-1)
    expert_mix = lax.optimization_barrier(jnp.sum(route_weight[:, :, None] * picked, axis=1))
    return (stream + expert_mix).astype(jnp.bfloat16)
```

```python
import functools

import jax
import jax.numpy as jnp
from jax import lax
from jax.experimental import pallas as pl
from jax.experimental.pallas import tpu as pltpu
from jax.sharding import PartitionSpec as P

epsilon = 1e-06
f32 = jnp.float32
bf16 = jnp.bfloat16
MESH = pl.DeviceIdType.MESH
GROUP = 8
AHEAD = 2


def layer_kernel(
    ep_count,
    tp_count,
    lengths,
    tokens_h,
    gain_h,
    post_h,
    wq_h,
    wk_h,
    wv_h,
    wf_h,
    wo_h,
    key_h,
    value_h,
    gate_h,
    routes_h,
    logits_h,
    wg_h,
    wu_h,
    wd_h,
    out,
    tokens,
    gain,
    post,
    wq,
    wkv,
    wf,
    wo,
    keys,
    values,
    gates,
    routes,
    logits,
    wg,
    wu,
    wd,
    query_rows,
    forget_rows,
    new_rows,
    fresh_values,
    mixed_rows,
    scores,
    probs,
    fresh_rows,
    total_rows,
    part_send,
    part_recv,
    pack_send,
    gathered,
    down_send,
    down_recv,
    ret_send,
    ret_recv,
    held,
    small_sem,
    pair_sem,
    cache_sem,
    part_ss,
    part_rs,
    pack_ss,
    pack_rs,
    fan_ss,
    fan_rs,
    fan_all,
    down_ss,
    down_rs,
    down_all,
    ret_ss,
    ret_rs,
):
    ep = lax.axis_index("ep")
    tp = lax.axis_index("tp")
    partner = tp + 1 - 2 * (tp % 2)
    chips = tp_count // 2
    seqs, width = tokens.shape
    heads = gates.shape[1]
    span = gates.shape[2]
    lanes = keys.shape[1]
    own = width // tp_count
    cap = pack_send.shape[1]
    slots = ep_count * cap
    hd = wq.shape[1] // heads
    per_lane = lanes // hd
    group_heads = heads // per_lane

    barrier = pltpu.get_barrier_semaphore()
    for o in range(1, tp_count):
        pl.semaphore_signal(
            barrier, inc=1, device_id={"tp": (tp + o) % tp_count}, device_id_type=MESH
        )

    def greet(k, c):
        pl.semaphore_signal(
            barrier, inc=1, device_id={"ep": (ep + k) % ep_count}, device_id_type=MESH
        )
        return c

    lax.fori_loop(1, ep_count, greet, 0)

    beside = len(wkv.shape) == 2
    pair_loads = [
        pltpu.make_async_copy(
            a, wkv.at[:, pl.ds(i * lanes, lanes)] if beside else wkv.at[i], pair_sem.at[0]
        )
        for i, a in enumerate([wk_h, wv_h])
    ]
    loads = [
        pltpu.make_async_copy(a, b, small_sem.at[i])
        for i, (a, b) in enumerate(
            [
                (tokens_h, tokens),
                (gain_h, gain),
                (wq_h, wq),
                (wf_h, wf),
                (routes_h, routes),
                (logits_h, logits),
                (post_h, post),
                (wo_h, wo),
                (wg_h, wg),
                (wu_h, wu),
                (wd_h, wd),
            ]
        )
    ]
    for c in [*loads[:3], *pair_loads, *loads[3:7]]:
        c.start()

    groups = seqs // GROUP

    def cache_load(kind, g):
        at = pl.ds(g * GROUP, GROUP)
        a, b = ((key_h, keys), (gate_h, gates), (value_h, values))[kind]
        return pltpu.make_async_copy(a.at[at], b.at[at], cache_sem.at[kind, g])

    def start_stage(g):
        def pick(ok, start):
            if isinstance(g, int):
                if ok:
                    start()
            else:
                pl.when(ok)(start)

        pick(g < groups, lambda: [cache_load(kind, g).start() for kind in (0, 1)] and None)
        pick((g > 0) & (g <= groups), lambda: cache_load(2, g - 1).start())
        for i in range(4):
            pick(g == groups + i, loads[7 + i].start)

    loads[0].wait()
    loads[1].wait()
    start_stage(0)
    wide = tokens[...].astype(f32)
    normed = (
        wide * lax.rsqrt(jnp.mean(wide * wide, axis=-1, keepdims=True) + epsilon) * gain[...]
    ).astype(bf16)
    for c in loads[2:4]:
        c.wait()
    pltpu.make_async_copy(wkv, wkv, pair_sem.at[0]).wait()
    start_stage(1)
    query = jnp.dot(normed, wq[...], preferred_element_type=f32).astype(bf16).astype(f32)
    query = query * hd ** (-0.5)
    if beside:
        fresh_pair = jnp.dot(normed, wkv[...], preferred_element_type=f32)
        fresh_pair = fresh_pair[:, :lanes], fresh_pair[:, lanes:]
    else:
        fresh_pair = [jnp.dot(normed, wkv[i], preferred_element_type=f32) for i in range(2)]
    fresh_key, fresh_value = [a.astype(bf16).astype(f32) for a in fresh_pair]
    fresh_values[...] = fresh_value
    forget_all = lax.dot_general(
        normed, wf[...], (((1,), (1,)), ((), ())), preferred_element_type=f32
    )
    forget = forget_all[:, 0:heads]
    for j in range(1, tp_count):
        forget = jnp.where(tp == j, forget_all[:, j * heads : (j + 1) * heads], forget)
    forget = jnp.minimum(forget, 0.0) - jnp.log1p(jnp.exp(-jnp.abs(forget)))
    lane_of = lax.broadcasted_iota(jnp.int32, (seqs, lanes), 1) // hd
    for h in range(heads):
        m, place, want = h // per_lane, h % per_lane, h // group_heads
        block = query[:, m * lanes : (m + 1) * lanes]
        if place != want:
            block = pltpu.roll(block, ((want - place) % per_lane) * hd, 1)
        block = jnp.where(lane_of == want, block, 0.0)
        at = pl.ds(h, seqs, stride=heads)
        query_rows[at, :] = block
        new_rows[at, :] = jnp.broadcast_to(
            jnp.sum(block * fresh_key, axis=-1, keepdims=True), (seqs, lanes)
        )
        forget_rows[at, :] = jnp.broadcast_to(forget[:, h : h + 1], (seqs, lanes))

    position = lax.broadcasted_iota(jnp.int32, (heads, span), 1)

    def rows_at(b):
        return pl.ds(pl.multiple_of(b * heads, heads), heads)

    def score(g):
        for i in range(GROUP):
            b = g * GROUP + i
            scores[g % 2, i] = jnp.dot(
                query_rows[rows_at(b), :].astype(bf16), keys[b], preferred_element_type=f32
            )

    def soften(g):
        for i in range(GROUP):
            b = g * GROUP + i
            length = lengths[b]
            gate = gates[b]
            latest = jnp.sum(
                jnp.where(position == length - 1, gate, 0.0), axis=-1, keepdims=True
            )
            fresh = new_rows[rows_at(b), :][:, 0:1]
            past = scores[g % 2, i] + (latest + forget_rows[rows_at(b), :][:, 0:1]) - gate
            past = jnp.where(position < length, past, -jnp.inf)
            peak = jnp.maximum(jnp.max(past, axis=-1, keepdims=True), fresh)
            past = jnp.exp(past - peak)
            fresh = jnp.exp(fresh - peak)
            total = jnp.sum(past, axis=-1, keepdims=True) + fresh
            probs[g % 2, i] = past.astype(bf16)
            fresh_rows[g % 2, i] = jnp.broadcast_to(fresh, (heads, lanes))
            total_rows[g % 2, i] = jnp.broadcast_to(total, (heads, lanes))

    def blend(g):
        for i in range(GROUP):
            b = g * GROUP + i
            mixed = lax.dot_general(
                probs[g % 2, i],
                values[b],
                (((1,), (1,)), ((), ())),
                preferred_element_type=f32,
            )
            mixed_rows[rows_at(b), :] = (
                mixed + fresh_rows[g % 2, i] * fresh_values[pl.ds(b, 1), :]
            ) / total_rows[g % 2, i]

    def arrived(kinds, g):
        for kind in kinds:
            cache_load(kind, g).wait()

    def attend(g, c):
        arrived((0, 1), g)
        arrived((2,), g - 2)
        start_stage(g + AHEAD)
        blend(g - 2)
        soften(g - 1)
        score(g)
        return c

    arrived((0, 1), 0)
    start_stage(AHEAD)
    score(0)
    arrived((0, 1), 1)
    start_stage(AHEAD + 1)
    soften(0)
    score(1)
    lax.fori_loop(2, groups, attend, 0)
    for g in range(groups + AHEAD, groups + 4):
        start_stage(g)
    arrived((2,), groups - 2)
    blend(groups - 2)
    soften(groups - 1)
    arrived((2,), groups - 1)
    blend(groups - 1)

    pieces = []
    for m in range(heads // per_lane):
        piece = jnp.zeros((seqs, lanes), f32)
        for place in range(per_lane):
            h = m * per_lane + place
            want = h // group_heads
            block = mixed_rows[pl.ds(h, seqs, stride=heads), :]
            if place != want:
                block = pltpu.roll(block, ((place - want) % per_lane) * hd, 1)
            piece = jnp.where(lane_of == place, block, piece)
        pieces.append(piece.astype(bf16))
    attended = jnp.concatenate(pieces, axis=1)

    loads[7].wait()
    for j in range(tp_count):
        part_send[j] = jnp.dot(
            attended, wo[:, j * own : (j + 1) * own], preferred_element_type=f32
        ).astype(bf16)
    pl.semaphore_wait(barrier, ep_count - 1 + tp_count - 1)

    def received(ref, sem):
        pltpu.make_async_copy(ref, ref, sem).wait()

    def part_copy(o):
        peer = (tp + o) % tp_count
        return pltpu.make_async_remote_copy(
            src_ref=part_send.at[peer],
            dst_ref=part_recv.at[o - 1],
            send_sem=part_ss.at[0],
            recv_sem=part_rs.at[0],
            device_id={"tp": peer},
            device_id_type=MESH,
        )

    part_copies = [part_copy(o) for o in range(1, tp_count)]
    for c in part_copies:
        c.start()
    for c in loads[4:7]:
        c.wait()
    slot = lax.broadcasted_iota(jnp.int32, (slots, seqs), 0)
    slot_expert, slot_rank = slot // cap, slot % cap
    first = routes[0:1, :] == slot_expert
    second = routes[1:2, :] == slot_expert
    named = jnp.where(jnp.logical_or(first, second), 1.0, 0.0)
    earlier = jnp.where(
        lax.broadcasted_iota(jnp.int32, (seqs, seqs), 0)
        < lax.broadcasted_iota(jnp.int32, (seqs, seqs), 1),
        1.0,
        0.0,
    )
    rank = jnp.dot(named.astype(bf16), earlier.astype(bf16), preferred_element_type=f32)
    chosen = jnp.where(rank == slot_rank.astype(f32), named, 0.0)
    dispatch = chosen.astype(bf16)
    one, two = logits[0:1, :], logits[1:2, :]
    top = jnp.maximum(one, two)
    e_one, e_two = jnp.exp(one - top), jnp.exp(two - top)
    share = jnp.where(first, e_one / (e_one + e_two), e_two / (e_one + e_two))
    weight = (share * chosen).T
    weight_high = weight.astype(bf16)
    weight_low = (weight - weight_high.astype(f32)).astype(bf16)

    columns = pl.ds(pl.multiple_of(tp * own, own), own)
    total = part_send[tp].astype(f32)
    received(part_recv, part_rs.at[0])
    for k in range(tp_count - 1):
        total = total + part_recv[k].astype(f32)
    residual = tokens[:, columns].astype(f32) + total

    packed = jnp.dot(dispatch, residual.astype(bf16), preferred_element_type=f32)
    for e in range(ep_count):
        pack_send[e] = packed[e * cap : (e + 1) * cap].astype(bf16)

    def pack_copy(k):
        return pltpu.make_async_remote_copy(
            src_ref=pack_send.at[(ep + k) % ep_count],
            dst_ref=gathered.at[tp, ep],
            send_sem=pack_ss.at[0],
            recv_sem=pack_rs.at[k],
            device_id={"ep": (ep + k) % ep_count},
            device_id_type=MESH,
        )

    def from_chip(base, d):
        return (base + tp_count - 2 * d) % tp_count

    def fan_copy(way, s):
        relayed = way - (chips - 1) if way >= chips else 0
        block = from_chip(tp, relayed) if relayed else tp
        return pltpu.make_async_remote_copy(
            src_ref=gathered.at[block, s],
            dst_ref=gathered.at[block, s],
            send_sem=fan_ss.at[0],
            recv_sem=fan_rs.at[way - 1, s] if 0 < way < chips else fan_all.at[max(0, relayed)],
            device_id={"tp": (tp + 2 * way) % tp_count if 0 < way < chips else partner},
            device_id_type=MESH,
        )

    def start_pack(k, c):
        pack_copy(k).start()
        return c

    lax.fori_loop(1, ep_count, start_pack, 0)
    gathered[tp, ep] = pack_send[ep]

    def fan_out(k, c):
        s = (ep + ep_count - k) % ep_count

        @pl.when(k > 0)
        def _():
            pack_copy(k).wait_recv()

        for way in [*range(1, chips), 0]:
            fan_copy(way, s).start()
        return c

    lax.fori_loop(0, ep_count, fan_out, 0)

    def relay(k, c):
        s = (ep + ep_count - k) % ep_count
        for way in range(1, chips):
            fan_copy(way, s).wait_recv()
            fan_copy(chips - 1 + way, s).start()
        return c

    for c in loads[8:]:
        c.wait()

    def rows_of(block):
        rows = jnp.concatenate(
            [gathered[block, s].astype(f32) for s in range(ep_count)], axis=0
        )
        at = pl.ds(pl.multiple_of(block * own, own), own)
        scaled = (rows * post[:, at]).astype(bf16)
        return (
            jnp.sum(rows * rows, axis=-1, keepdims=True),
            jnp.dot(scaled, wg[at, :], preferred_element_type=f32),
            jnp.dot(scaled, wu[at, :], preferred_element_type=f32),
        )

    def arrive(relayed):
        received(gathered.at[0], fan_all.at[relayed])

    def add(a, b):
        return tuple(x + y for x, y in zip(a, b))

    sums = rows_of(tp)
    lax.fori_loop(0, ep_count, relay, 0)
    arrive(0)
    sums = add(sums, rows_of(partner))
    for d in range(1, chips):
        sums = add(sums, rows_of(from_chip(tp, d)))
    for d in range(1, chips):
        arrive(d)
        sums = add(sums, rows_of(from_chip(partner, d)))
    squares, gate_act, upper = sums
    scale = lax.rsqrt(squares / width + epsilon)
    gate_act = gate_act * scale
    hidden = (gate_act / (1.0 + jnp.exp(-gate_act)) * (upper * scale)).astype(bf16)

    def down(block):
        at = pl.ds(pl.multiple_of(block * own, own), own)
        return jnp.dot(hidden, wd[:, at], preferred_element_type=f32)

    def down_copy(k, e):
        return pltpu.make_async_remote_copy(
            src_ref=down_send.at[k, e],
            dst_ref=down_recv.at[k, e],
            send_sem=down_ss.at[0],
            recv_sem=down_rs.at[k, e] if k < chips - 1 else down_all.at[e],
            device_id={
                "tp": (tp + 2 * (k - chips + 1)) % tp_count if k >= chips else partner
            },
            device_id_type=MESH,
        )

    def turn(k):
        return (ep + 1 + k) % ep_count

    def spread(ref, rows):
        for e in range(ep_count):
            ref[e] = rows[e * cap : (e + 1) * cap].astype(ref.dtype)

    def start_down(way):
        def one(k, c):
            down_copy(way, turn(k)).start()
            return c

        lax.fori_loop(0, ep_count, one, 0)

    def ret_copy(k):
        return pltpu.make_async_remote_copy(
            src_ref=ret_send.at[(ep + k) % ep_count],
            dst_ref=ret_recv.at[ep],
            send_sem=ret_ss.at[0],
            recv_sem=ret_rs.at[0],
            device_id={"ep": (ep + k) % ep_count},
            device_id_type=MESH,
        )

    for d in range(1, chips):
        spread(down_send.at[d - 1], down((partner + 2 * d) % tp_count))
        start_down(d - 1)
    for d in range(1, chips):
        spread(held, down((tp + 2 * d) % tp_count))

        def cross(k, c):
            e = turn(k)
            down_copy(d - 1, e).wait_recv()
            down_send[chips - 1 + d, e] = (
                held[e] + down_recv[d - 1, e].astype(f32)
            ).astype(bf16)
            down_copy(chips - 1 + d, e).start()
            return c

        lax.fori_loop(0, ep_count, cross, 0)
    spread(down_send.at[chips - 1], down(partner))
    start_down(chips - 1)
    spread(held, down(tp))

    def give_back(k, c):
        e = turn(k)
        total = held[e]
        received(down_recv.at[pl.ds(chips - 1, chips), e], down_all.at[e])
        for way in range(chips - 1, 2 * chips - 1):
            total = total + down_recv[way, e].astype(f32)

        @pl.when(k < ep_count - 1)
        def _():
            ret_send[e] = total.astype(bf16)
            ret_copy(k + 1).start()

        @pl.when(k == ep_count - 1)
        def _():
            ret_recv[e] = total.astype(bf16)

        return c

    lax.fori_loop(0, ep_count, give_back, 0)

    received(ret_recv.at[pl.ds(0, ep_count - 1)], ret_rs.at[0])
    returned = jnp.concatenate(
        [ret_recv[e].astype(f32) for e in range(ep_count)], axis=0
    ).astype(bf16)
    mix = jnp.dot(weight_high, returned, preferred_element_type=f32) + jnp.dot(
        weight_low, returned, preferred_element_type=f32
    )
    out[...] = (residual + mix).astype(bf16)

    received(part_recv, part_ss.at[0])
    received(ret_recv.at[pl.ds(0, ep_count - 1)], pack_ss.at[0])
    received(ret_recv.at[pl.ds(0, ep_count - 1)], ret_ss.at[0])
    received(down_recv, fan_ss.at[0])
    received(down_recv, down_ss.at[0])


def body(
    tokens,
    norm_gain,
    post_gain,
    w_query,
    w_key,
    w_value,
    w_forget,
    w_output,
    key_cache,
    value_cache,
    gate_cache,
    lengths,
    routes,
    route_logits,
    w_gate,
    w_up,
    w_down,
):
    ep_count = lax.axis_size("ep")
    tp_count = lax.axis_size("tp")
    ways = tp_count - 1
    seqs, width = tokens.shape
    heads, span = gate_cache.shape[1:]
    own = width // tp_count
    cap = 2 * seqs * routes.shape[1] // ep_count
    lanes = key_cache.shape[1] * key_cache.shape[2]
    hbm = [
        tokens,
        norm_gain.reshape(1, width),
        post_gain.reshape(1, width),
        w_query,
        w_key,
        w_value,
        w_forget.T,
        w_output,
        key_cache.reshape(seqs, lanes, span),
        value_cache.reshape(seqs, lanes, span),
        gate_cache,
        routes.T,
        route_logits.T,
        w_gate.reshape(w_gate.shape[1:]),
        w_up.reshape(w_up.shape[1:]),
        w_down.reshape(w_down.shape[1:]),
    ]
    dma = pltpu.SemaphoreType.DMA
    pair = (width, 2 * lanes) if lanes % 128 == 0 else (2, width, lanes)
    scratch = [
        pltpu.VMEM(pair if a is w_key else a.shape, a.dtype) for a in hbm if a is not w_value
    ] + [
        pltpu.VMEM((seqs * heads, lanes), f32),
        pltpu.VMEM((seqs * heads, lanes), f32),
        pltpu.VMEM((seqs * heads, lanes), f32),
        pltpu.VMEM((seqs, lanes), f32),
        pltpu.VMEM((seqs * heads, lanes), f32),
        pltpu.VMEM((2, GROUP, heads, span), f32),
        pltpu.VMEM((2, GROUP, heads, span), bf16),
        pltpu.VMEM((2, GROUP, heads, lanes), f32),
        pltpu.VMEM((2, GROUP, heads, lanes), f32),
        pltpu.VMEM((tp_count, seqs, own), bf16),
        pltpu.VMEM((ways, seqs, own), bf16),
        pltpu.VMEM((ep_count, cap, own), bf16),
        pltpu.VMEM((tp_count, ep_count, cap, own), bf16),
        pltpu.VMEM((ways, ep_count, cap, own), bf16),
        pltpu.VMEM((ways, ep_count, cap, own), bf16),
        pltpu.VMEM((ep_count, cap, own), bf16),
        pltpu.VMEM((ep_count, cap, own), bf16),
        pltpu.VMEM((ep_count, cap, own), f32),
        dma((11,)),
        dma((1,)),
        dma((3, seqs // GROUP)),
        dma((1,)),
        dma((1,)),
        dma((1,)),
        dma((ep_count,)),
        dma((1,)),
        dma((tp_count // 2 - 1, ep_count)),
        dma((tp_count // 2,)),
        dma((1,)),
        dma((tp_count // 2 - 1, ep_count)),
        dma((ep_count,)),
        dma((1,)),
        dma((1,)),
    ]
    return pl.pallas_call(
        functools.partial(layer_kernel, ep_count, tp_count),
        out_shape=pltpu.VMEM((seqs, own), bf16),
        in_specs=[pl.BlockSpec(memory_space=pltpu.SMEM)]
        + [pl.BlockSpec(memory_space=pl.ANY)] * len(hbm),
        out_specs=pl.BlockSpec(memory_space=pltpu.VMEM),
        scratch_shapes=scratch,
        compiler_params=pltpu.CompilerParams(
            collective_id=0, has_side_effects=True, vmem_limit_bytes=48 * 1024 * 1024
        ),
    )(*[pltpu.with_memory_space_constraint(a, pltpu.HBM) for a in [lengths, *hbm]])


def solution(mesh):
    in_specs = (
        P("ep", None),
        P(),
        P(),
        P(None, "tp"),
        P(None, "tp"),
        P(None, "tp"),
        P(),
        P("tp", None),
        P("ep", "tp", None, None),
        P("ep", "tp", None, None),
        P("ep", "tp", None),
        P("ep"),
        P("ep", None),
        P("ep", None),
        P("ep", None, "tp"),
        P("ep", None, "tp"),
        P("ep", "tp", None),
    )
    out_specs = P("ep", "tp")
    return jax.shard_map(body, mesh=mesh, in_specs=in_specs, out_specs=out_specs, check_vma=False)
```

```python
import functools

import jax
import jax.numpy as jnp
from jax import lax
from jax.experimental import pallas as pl
from jax.experimental.pallas import tpu as pltpu
from jax.sharding import PartitionSpec as P

epsilon = 1e-06
f32 = jnp.float32
bf16 = jnp.bfloat16
MESH = pl.DeviceIdType.MESH
GROUP = 8
AHEAD = 4


def layer_kernel(
    ep_count,
    tp_count,
    lengths,
    tokens_h,
    gain_h,
    post_h,
    wq_h,
    wk_h,
    wv_h,
    wf_h,
    wo_h,
    key_h,
    value_h,
    gate_h,
    routes_h,
    logits_h,
    wg_h,
    wu_h,
    wd_h,
    out,
    tokens,
    gain,
    post,
    wq,
    wkv,
    wf,
    wo,
    keys,
    values,
    gates,
    routes,
    logits,
    wgu,
    wd,
    query_rows,
    forget_rows,
    fresh_keys,
    fresh_values,
    mixed_rows,
    scores,
    probs,
    fresh_rows,
    total_rows,
    part_send,
    part_recv,
    pack_send,
    gathered,
    down_send,
    down_recv,
    ret_send,
    ret_recv,
    held,
    small_sem,
    pair_sem,
    cache_sem,
    part_ss,
    part_rs,
    pack_ss,
    pack_rs,
    fan_ss,
    fan_rs,
    fan_all,
    down_ss,
    down_rs,
    down_all,
    ret_ss,
    ret_rs,
):
    ep = lax.axis_index("ep")
    tp = lax.axis_index("tp")
    partner = tp + 1 - 2 * (tp % 2)
    chips = tp_count // 2
    seqs, width = tokens.shape
    heads = gates.shape[1]
    span = gates.shape[2]
    lanes = keys.shape[1]
    own = width // tp_count
    cap = pack_send.shape[1]
    slots = ep_count * cap
    hd = wq.shape[1] // heads
    per_lane = lanes // hd
    group_heads = heads // per_lane

    barrier = pltpu.get_barrier_semaphore()
    for o in range(1, tp_count):
        pl.semaphore_signal(
            barrier, inc=1, device_id={"tp": (tp + o) % tp_count}, device_id_type=MESH
        )

    def greet(k, c):
        pl.semaphore_signal(
            barrier, inc=1, device_id={"ep": (ep + k) % ep_count}, device_id_type=MESH
        )
        return c

    lax.fori_loop(1, ep_count, greet, 0)

    beside = len(wkv.shape) == 2
    pair_loads = [
        pltpu.make_async_copy(
            a, wkv.at[:, pl.ds(i * lanes, lanes)] if beside else wkv.at[i], pair_sem.at[0]
        )
        for i, a in enumerate([wk_h, wv_h])
    ]
    inner = wg_h.shape[1]
    joined = len(wgu.shape) == 2
    expert_loads = [
        pltpu.make_async_copy(
            a, wgu.at[:, pl.ds(i * inner, inner)] if joined else wgu.at[i], pair_sem.at[1]
        )
        for i, a in enumerate([wg_h, wu_h])
    ]
    loads = [
        pltpu.make_async_copy(a, b, small_sem.at[i])
        for i, (a, b) in enumerate(
            [
                (tokens_h, tokens),
                (gain_h, gain),
                (wq_h, wq),
                (wf_h, wf),
                (routes_h, routes),
                (logits_h, logits),
                (post_h, post),
                (wo_h, wo),
                (wd_h, wd),
            ]
        )
    ]
    for c in [*loads[:3], *pair_loads, *loads[3:7]]:
        c.start()

    groups = seqs // GROUP

    def cache_load(kind, g):
        at = pl.ds(g * GROUP, GROUP)
        a, b = ((key_h, keys), (gate_h, gates), (value_h, values))[kind]
        return pltpu.make_async_copy(a.at[at], b.at[at], cache_sem.at[kind, g])

    def start_stage(g):
        def pick(ok, start):
            if isinstance(g, int):
                if ok:
                    start()
            else:
                pl.when(ok)(start)

        pick(g < groups, lambda: [cache_load(kind, g).start() for kind in (0, 1)] and None)
        pick((g > 0) & (g <= groups), lambda: cache_load(2, g - 1).start())
        for i, load in enumerate([loads[7], *expert_loads, loads[8]]):
            pick(g == groups + i, load.start)

    start_stage(0)
    loads[0].wait()
    loads[1].wait()
    start_stage(1)
    wide = tokens[...].astype(f32)
    normed = (
        wide * lax.rsqrt(jnp.mean(wide * wide, axis=-1, keepdims=True) + epsilon) * gain[...]
    ).astype(bf16)
    for c in loads[2:4]:
        c.wait()
    pltpu.make_async_copy(wkv, wkv, pair_sem.at[0]).wait()
    start_stage(2)
    start_stage(3)
    query = jnp.dot(normed, wq[...], preferred_element_type=f32).astype(bf16).astype(f32)
    query = query * hd ** (-0.5)
    if beside:
        fresh_pair = jnp.dot(normed, wkv[...], preferred_element_type=f32)
        fresh_pair = fresh_pair[:, :lanes], fresh_pair[:, lanes:]
    else:
        fresh_pair = [jnp.dot(normed, wkv[i], preferred_element_type=f32) for i in range(2)]
    fresh_key, fresh_value = [a.astype(bf16).astype(f32) for a in fresh_pair]
    fresh_values[...] = fresh_value
    fresh_keys[...] = fresh_key
    forget_all = lax.dot_general(
        normed, wf[...], (((1,), (1,)), ((), ())), preferred_element_type=f32
    )
    forget = forget_all[:, 0:heads]
    for j in range(1, tp_count):
        forget = jnp.where(tp == j, forget_all[:, j * heads : (j + 1) * heads], forget)
    forget = jnp.minimum(forget, 0.0) - jnp.log1p(jnp.exp(-jnp.abs(forget)))
    lane_of = lax.broadcasted_iota(jnp.int32, (seqs, lanes), 1) // hd
    for h in range(heads):
        m, place, want = h // per_lane, h % per_lane, h // group_heads
        block = query[:, m * lanes : (m + 1) * lanes]
        if place != want:
            block = pltpu.roll(block, ((want - place) % per_lane) * hd, 1)
        block = jnp.where(lane_of == want, block, 0.0)
        at = pl.ds(h, seqs, stride=heads)
        query_rows[at, :] = block
        forget_rows[at, :] = jnp.broadcast_to(forget[:, h : h + 1], (seqs, lanes))

    position = lax.broadcasted_iota(jnp.int32, (heads, span), 1)

    def rows_at(b):
        return pl.ds(pl.multiple_of(b * heads, heads), heads)

    def score(g):
        for i in range(GROUP):
            b = g * GROUP + i
            scores[g % 2, i] = jnp.dot(
                query_rows[rows_at(b), :].astype(bf16), keys[b], preferred_element_type=f32
            )

    def soften(g):
        for i in range(GROUP):
            b = g * GROUP + i
            length = lengths[b]
            gate = gates[b]
            latest = jnp.sum(
                jnp.where(position == length - 1, gate, 0.0), axis=-1, keepdims=True
            )
            fresh = jnp.sum(
                query_rows[rows_at(b), :] * fresh_keys[pl.ds(b, 1), :], axis=-1, keepdims=True
            )
            past = scores[g % 2, i] + (latest + forget_rows[rows_at(b), :][:, 0:1]) - gate
            past = jnp.where(position < length, past, -jnp.inf)
            peak = jnp.maximum(jnp.max(past, axis=-1, keepdims=True), fresh)
            past = jnp.exp(past - peak)
            fresh = jnp.exp(fresh - peak)
            total = jnp.sum(past, axis=-1, keepdims=True) + fresh
            probs[g % 2, i] = past.astype(bf16)
            fresh_rows[g % 2, i] = jnp.broadcast_to(fresh, (heads, lanes))
            total_rows[g % 2, i] = jnp.broadcast_to(total, (heads, lanes))

    def blend(g):
        for i in range(GROUP):
            b = g * GROUP + i
            mixed = lax.dot_general(
                probs[g % 2, i],
                values[b],
                (((1,), (1,)), ((), ())),
                preferred_element_type=f32,
            )
            mixed_rows[rows_at(b), :] = (
                mixed + fresh_rows[g % 2, i] * fresh_values[pl.ds(b, 1), :]
            ) / total_rows[g % 2, i]

    def arrived(kinds, g):
        for kind in kinds:
            cache_load(kind, g).wait()

    def attend(g, c):
        arrived((0, 1), g)
        arrived((2,), g - 2)
        start_stage(g + AHEAD)
        blend(g - 2)
        soften(g - 1)
        score(g)
        return c

    arrived((0, 1), 0)
    start_stage(AHEAD)
    score(0)
    arrived((0, 1), 1)
    start_stage(AHEAD + 1)
    soften(0)
    score(1)
    lax.fori_loop(2, groups, attend, 0)
    for g in range(groups + AHEAD, groups + 4):
        start_stage(g)
    arrived((2,), groups - 2)
    blend(groups - 2)
    soften(groups - 1)
    arrived((2,), groups - 1)
    blend(groups - 1)

    pieces = []
    for m in range(heads // per_lane):
        piece = jnp.zeros((seqs, lanes), f32)
        for place in range(per_lane):
            h = m * per_lane + place
            want = h // group_heads
            block = mixed_rows[pl.ds(h, seqs, stride=heads), :]
            if place != want:
                block = pltpu.roll(block, ((place - want) % per_lane) * hd, 1)
            piece = jnp.where(lane_of == place, block, piece)
        pieces.append(piece.astype(bf16))
    attended = jnp.concatenate(pieces, axis=1)

    loads[7].wait()
    pl.semaphore_wait(barrier, ep_count - 1 + tp_count - 1)

    def project(peer):
        at = pl.ds(pl.multiple_of(peer * own, own), own)
        part_send[peer] = jnp.dot(
            attended, wo[:, at], preferred_element_type=f32
        ).astype(bf16)

    def received(ref, sem):
        pltpu.make_async_copy(ref, ref, sem).wait()

    def part_copy(peer):
        o = (peer + tp_count - tp) % tp_count
        return pltpu.make_async_remote_copy(
            src_ref=part_send.at[peer],
            dst_ref=part_recv.at[o - 1],
            send_sem=part_ss.at[0],
            recv_sem=part_rs.at[0],
            device_id={"tp": peer},
            device_id_type=MESH,
        )

    for d in [*range(1, chips), 0]:
        for base in (tp, partner):
            if d or base is partner:
                peer = (base + 2 * d) % tp_count
                project(peer)
                part_copy(peer).start()
    project(tp)
    for c in loads[4:7]:
        c.wait()
    slot = lax.broadcasted_iota(jnp.int32, (slots, seqs), 0)
    slot_expert, slot_rank = slot // cap, slot % cap
    first = routes[0:1, :] == slot_expert
    second = routes[1:2, :] == slot_expert
    named = jnp.where(jnp.logical_or(first, second), 1.0, 0.0)
    earlier = jnp.where(
        lax.broadcasted_iota(jnp.int32, (seqs, seqs), 0)
        < lax.broadcasted_iota(jnp.int32, (seqs, seqs), 1),
        1.0,
        0.0,
    )
    rank = jnp.dot(named.astype(bf16), earlier.astype(bf16), preferred_element_type=f32)
    chosen = jnp.where(rank == slot_rank.astype(f32), named, 0.0)
    dispatch = chosen.astype(bf16)
    one, two = logits[0:1, :], logits[1:2, :]
    top = jnp.maximum(one, two)
    e_one, e_two = jnp.exp(one - top), jnp.exp(two - top)
    share = jnp.where(first, e_one / (e_one + e_two), e_two / (e_one + e_two))
    weight = (share * chosen).T
    weight_high = weight.astype(bf16)
    weight_low = (weight - weight_high.astype(f32)).astype(bf16)
    weight_both = jnp.concatenate([weight_high, weight_low], axis=0)

    columns = pl.ds(pl.multiple_of(tp * own, own), own)
    total = part_send[tp].astype(f32)
    received(part_recv, part_rs.at[0])
    for k in range(tp_count - 1):
        total = total + part_recv[k].astype(f32)
    residual = tokens[:, columns].astype(f32) + total

    packed = jnp.dot(dispatch, residual.astype(bf16), preferred_element_type=f32)
    for e in range(ep_count):
        pack_send[e] = packed[e * cap : (e + 1) * cap].astype(bf16)

    paired = ep_count & (ep_count - 1) == 0

    def across(k):
        if not paired:
            return (ep + k) % ep_count
        e, bit = 0, 1
        while bit < ep_count:
            e, bit = e + (ep // bit + k // bit) % 2 * bit, 2 * bit
        return e

    def source(k):
        return across(k) if paired else (ep + ep_count - k) % ep_count

    def pack_copy(k):
        return pltpu.make_async_remote_copy(
            src_ref=pack_send.at[across(k)],
            dst_ref=gathered.at[tp, ep],
            send_sem=pack_ss.at[0],
            recv_sem=pack_rs.at[k],
            device_id={"ep": across(k)},
            device_id_type=MESH,
        )

    def from_chip(base, d):
        return (base + tp_count - 2 * d) % tp_count

    def fan_copy(way, s):
        relayed = way - (chips - 1) if way >= chips else 0
        block = from_chip(tp, relayed) if relayed else tp
        return pltpu.make_async_remote_copy(
            src_ref=gathered.at[block, s],
            dst_ref=gathered.at[block, s],
            send_sem=fan_ss.at[0],
            recv_sem=fan_rs.at[way - 1, s] if 0 < way < chips else fan_all.at[max(0, relayed)],
            device_id={"tp": (tp + 2 * way) % tp_count if 0 < way < chips else partner},
            device_id_type=MESH,
        )

    def start_pack(k, c):
        pack_copy(k).start()
        return c

    lax.fori_loop(1, ep_count, start_pack, 0)
    gathered[tp, ep] = pack_send[ep]

    def fan_out(k, c):
        s = source(k)

        @pl.when(k > 0)
        def _():
            pack_copy(k).wait_recv()

        for way in [*range(1, chips), 0]:
            fan_copy(way, s).start()
        return c

    lax.fori_loop(0, ep_count, fan_out, 0)

    def relay(k, c):
        s = source(k)
        for way in range(1, chips):
            fan_copy(way, s).wait_recv()
            fan_copy(chips - 1 + way, s).start()
        return c

    received(wgu, pair_sem.at[1])
    loads[8].wait()

    def rows_of(block):
        rows = jnp.concatenate(
            [gathered[block, s].astype(f32) for s in range(ep_count)], axis=0
        )
        at = pl.ds(pl.multiple_of(block * own, own), own)
        scaled = (rows * post[:, at]).astype(bf16)
        squares = jnp.sum(rows * rows, axis=-1, keepdims=True)
        if joined:
            both = jnp.dot(scaled, wgu[at, :], preferred_element_type=f32)
            return squares, both[:, :inner], both[:, inner:]
        return squares, *[
            jnp.dot(scaled, wgu[i, at, :], preferred_element_type=f32) for i in range(2)
        ]

    def arrive(relayed):
        received(gathered.at[0], fan_all.at[relayed])

    def add(a, b):
        return tuple(x + y for x, y in zip(a, b))

    sums = rows_of(tp)
    lax.fori_loop(0, ep_count, relay, 0)
    arrive(0)
    sums = add(sums, rows_of(partner))
    for d in range(1, chips):
        sums = add(sums, rows_of(from_chip(tp, d)))
    for d in range(1, chips):
        arrive(d)
        sums = add(sums, rows_of(from_chip(partner, d)))
    squares, gate_act, upper = sums
    scale = lax.rsqrt(squares / width + epsilon)
    gate_act = gate_act * scale
    hidden = (gate_act / (1.0 + jnp.exp(-gate_act)) * (upper * scale)).astype(bf16)

    def down(block):
        at = pl.ds(pl.multiple_of(block * own, own), own)
        return jnp.dot(hidden, wd[:, at], preferred_element_type=f32)

    def down_copy(k, e):
        return pltpu.make_async_remote_copy(
            src_ref=down_send.at[k, e],
            dst_ref=down_recv.at[k, e],
            send_sem=down_ss.at[0],
            recv_sem=down_rs.at[k, e] if k < chips - 1 else down_all.at[e],
            device_id={
                "tp": (tp + 2 * (k - chips + 1)) % tp_count if k >= chips else partner
            },
            device_id_type=MESH,
        )

    def turn(k):
        return across(ep_count - 1 - k)

    def spread(ref, rows):
        for e in range(ep_count):
            ref[e] = rows[e * cap : (e + 1) * cap].astype(ref.dtype)

    def start_down(way):
        def one(k, c):
            down_copy(way, turn(k)).start()
            return c

        lax.fori_loop(0, ep_count, one, 0)

    def ret_copy(k):
        return pltpu.make_async_remote_copy(
            src_ref=ret_send.at[across(k)],
            dst_ref=ret_recv.at[ep],
            send_sem=ret_ss.at[0],
            recv_sem=ret_rs.at[0],
            device_id={"ep": across(k)},
            device_id_type=MESH,
        )

    for d in range(1, chips):
        spread(down_send.at[d - 1], down((partner + 2 * d) % tp_count))
        start_down(d - 1)
    for d in range(1, chips):
        spread(held, down((tp + 2 * d) % tp_count))

        def cross(k, c):
            e = turn(k)
            down_copy(d - 1, e).wait_recv()
            down_send[chips - 1 + d, e] = (
                held[e] + down_recv[d - 1, e].astype(f32)
            ).astype(bf16)
            down_copy(chips - 1 + d, e).start()
            return c

        lax.fori_loop(0, ep_count, cross, 0)
    spread(down_send.at[chips - 1], down(partner))
    start_down(chips - 1)
    spread(held, down(tp))

    def give_back(k, c):
        e = turn(k)
        total = held[e]
        received(down_recv.at[pl.ds(chips - 1, chips), e], down_all.at[e])
        for way in range(chips - 1, 2 * chips - 1):
            total = total + down_recv[way, e].astype(f32)

        @pl.when(k < ep_count - 1)
        def _():
            ret_send[e] = total.astype(bf16)
            ret_copy(ep_count - 1 - k).start()

        @pl.when(k == ep_count - 1)
        def _():
            ret_recv[e] = total.astype(bf16)

        return c

    lax.fori_loop(0, ep_count, give_back, 0)

    received(ret_recv.at[pl.ds(0, ep_count - 1)], ret_rs.at[0])
    returned = jnp.concatenate(
        [ret_recv[e].astype(f32) for e in range(ep_count)], axis=0
    ).astype(bf16)
    mix = jnp.dot(weight_both, returned, preferred_element_type=f32)
    out[...] = (residual + (mix[:seqs] + mix[seqs:])).astype(bf16)

    received(part_recv, part_ss.at[0])
    received(ret_recv.at[pl.ds(0, ep_count - 1)], pack_ss.at[0])
    received(ret_recv.at[pl.ds(0, ep_count - 1)], ret_ss.at[0])
    received(down_recv, fan_ss.at[0])
    received(down_recv, down_ss.at[0])


def body(
    tokens,
    norm_gain,
    post_gain,
    w_query,
    w_key,
    w_value,
    w_forget,
    w_output,
    key_cache,
    value_cache,
    gate_cache,
    lengths,
    routes,
    route_logits,
    w_gate,
    w_up,
    w_down,
):
    ep_count = lax.axis_size("ep")
    tp_count = lax.axis_size("tp")
    ways = tp_count - 1
    seqs, width = tokens.shape
    heads, span = gate_cache.shape[1:]
    own = width // tp_count
    cap = 2 * seqs * routes.shape[1] // ep_count
    lanes = key_cache.shape[1] * key_cache.shape[2]
    hbm = [
        tokens,
        norm_gain.reshape(1, width),
        post_gain.reshape(1, width),
        w_query,
        w_key,
        w_value,
        w_forget.T,
        w_output,
        key_cache.reshape(seqs, lanes, span),
        value_cache.reshape(seqs, lanes, span),
        gate_cache,
        routes.T,
        route_logits.T,
        w_gate.reshape(w_gate.shape[1:]),
        w_up.reshape(w_up.shape[1:]),
        w_down.reshape(w_down.shape[1:]),
    ]
    dma = pltpu.SemaphoreType.DMA
    def beside(a):
        rows, columns = a.shape
        return (rows, 2 * columns) if columns % 128 == 0 else (2, rows, columns)

    gate_up = hbm[13:15]
    scratch = [
        pltpu.VMEM(beside(a) if a is w_key or a is gate_up[0] else a.shape, a.dtype)
        for a in hbm
        if a is not w_value and a is not gate_up[1]
    ] + [
        pltpu.VMEM((seqs * heads, lanes), f32),
        pltpu.VMEM((seqs * heads, lanes), f32),
        pltpu.VMEM((seqs, lanes), f32),
        pltpu.VMEM((seqs, lanes), f32),
        pltpu.VMEM((seqs * heads, lanes), f32),
        pltpu.VMEM((2, GROUP, heads, span), f32),
        pltpu.VMEM((2, GROUP, heads, span), bf16),
        pltpu.VMEM((2, GROUP, heads, lanes), f32),
        pltpu.VMEM((2, GROUP, heads, lanes), f32),
        pltpu.VMEM((tp_count, seqs, own), bf16),
        pltpu.VMEM((ways, seqs, own), bf16),
        pltpu.VMEM((ep_count, cap, own), bf16),
        pltpu.VMEM((tp_count, ep_count, cap, own), bf16),
        pltpu.VMEM((ways, ep_count, cap, own), bf16),
        pltpu.VMEM((ways, ep_count, cap, own), bf16),
        pltpu.VMEM((ep_count, cap, own), bf16),
        pltpu.VMEM((ep_count, cap, own), bf16),
        pltpu.VMEM((ep_count, cap, own), f32),
        dma((9,)),
        dma((2,)),
        dma((3, seqs // GROUP)),
        dma((1,)),
        dma((1,)),
        dma((1,)),
        dma((ep_count,)),
        dma((1,)),
        dma((tp_count // 2 - 1, ep_count)),
        dma((tp_count // 2,)),
        dma((1,)),
        dma((tp_count // 2 - 1, ep_count)),
        dma((ep_count,)),
        dma((1,)),
        dma((1,)),
    ]
    return pl.pallas_call(
        functools.partial(layer_kernel, ep_count, tp_count),
        out_shape=pltpu.VMEM((seqs, own), bf16),
        in_specs=[pl.BlockSpec(memory_space=pltpu.SMEM)]
        + [pl.BlockSpec(memory_space=pl.ANY)] * len(hbm),
        out_specs=pl.BlockSpec(memory_space=pltpu.VMEM),
        scratch_shapes=scratch,
        compiler_params=pltpu.CompilerParams(
            collective_id=0, has_side_effects=True, vmem_limit_bytes=48 * 1024 * 1024
        ),
    )(*[pltpu.with_memory_space_constraint(a, pltpu.HBM) for a in [lengths, *hbm]])


def solution(mesh):
    in_specs = (
        P("ep", None),
        P(),
        P(),
        P(None, "tp"),
        P(None, "tp"),
        P(None, "tp"),
        P(),
        P("tp", None),
        P("ep", "tp", None, None),
        P("ep", "tp", None, None),
        P("ep", "tp", None),
        P("ep"),
        P("ep", None),
        P("ep", None),
        P("ep", None, "tp"),
        P("ep", None, "tp"),
        P("ep", "tp", None),
    )
    out_specs = P("ep", "tp")
    return jax.shard_map(body, mesh=mesh, in_specs=in_specs, out_specs=out_specs, check_vma=False)
```

```python
import functools

import jax
import jax.numpy as jnp
from jax import lax
from jax.experimental import pallas as pl
from jax.experimental.pallas import tpu as pltpu
from jax.sharding import PartitionSpec as P

epsilon = 1e-06
f32 = jnp.float32
bf16 = jnp.bfloat16
MESH = pl.DeviceIdType.MESH
GROUP = 8
AHEAD = 4


def layer_kernel(
    ep_count,
    tp_count,
    lengths,
    tokens_h,
    gain_h,
    post_h,
    wq_h,
    wk_h,
    wv_h,
    wf_h,
    wo_h,
    key_h,
    value_h,
    gate_h,
    routes_h,
    logits_h,
    wg_h,
    wu_h,
    wd_h,
    out,
    tokens,
    gain,
    post,
    wq,
    wkv,
    wf,
    wo,
    keys,
    values,
    gates,
    routes,
    logits,
    wgu,
    wd,
    query_rows,
    forget_rows,
    fresh_keys,
    fresh_values,
    mixed_rows,
    scores,
    probs,
    fresh_rows,
    total_rows,
    part_send,
    part_recv,
    pack_send,
    gathered,
    down_send,
    down_recv,
    ret_send,
    ret_recv,
    held,
    small_sem,
    pair_sem,
    cache_sem,
    part_ss,
    part_rs,
    pack_ss,
    pack_rs,
    fan_ss,
    fan_rs,
    fan_all,
    down_ss,
    down_rs,
    down_all,
    ret_ss,
    ret_rs,
):
    ep = lax.axis_index("ep")
    tp = lax.axis_index("tp")
    partner = tp + 1 - 2 * (tp % 2)
    chips = tp_count // 2
    seqs, width = tokens.shape
    heads = gates.shape[1]
    span = gates.shape[2]
    lanes = keys.shape[1]
    own = width // tp_count
    cap = pack_send.shape[1]
    slots = ep_count * cap
    hd = wq.shape[1] // heads
    per_lane = lanes // hd
    group_heads = heads // per_lane

    barrier = pltpu.get_barrier_semaphore()
    for o in range(1, tp_count):
        pl.semaphore_signal(
            barrier, inc=1, device_id={"tp": (tp + o) % tp_count}, device_id_type=MESH
        )

    def greet(k, c):
        pl.semaphore_signal(
            barrier, inc=1, device_id={"ep": (ep + k) % ep_count}, device_id_type=MESH
        )
        return c

    lax.fori_loop(1, ep_count, greet, 0)

    beside = len(wkv.shape) == 2
    pair_loads = [
        pltpu.make_async_copy(
            a, wkv.at[:, pl.ds(i * lanes, lanes)] if beside else wkv.at[i], pair_sem.at[0]
        )
        for i, a in enumerate([wk_h, wv_h])
    ]
    inner = wg_h.shape[1]
    joined = len(wgu.shape) == 2
    expert_loads = [
        pltpu.make_async_copy(
            a, wgu.at[:, pl.ds(i * inner, inner)] if joined else wgu.at[i], pair_sem.at[1]
        )
        for i, a in enumerate([wg_h, wu_h])
    ]
    loads = [
        pltpu.make_async_copy(a, b, small_sem.at[i])
        for i, (a, b) in enumerate(
            [
                (tokens_h, tokens),
                (gain_h, gain),
                (wq_h, wq),
                (wf_h, wf),
                (routes_h, routes),
                (logits_h, logits),
                (post_h, post),
                (wo_h, wo),
                (wd_h, wd),
            ]
        )
    ]
    for c in [*loads[:3], *pair_loads, *loads[3:7]]:
        c.start()

    groups = seqs // GROUP

    def cache_load(kind, g):
        at = pl.ds(g * GROUP, GROUP)
        a, b = ((key_h, keys), (gate_h, gates), (value_h, values))[kind]
        return pltpu.make_async_copy(a.at[at], b.at[at], cache_sem.at[kind, g])

    def start_stage(g):
        def pick(ok, start):
            if isinstance(g, int):
                if ok:
                    start()
            else:
                pl.when(ok)(start)

        pick(g < groups, lambda: [cache_load(kind, g).start() for kind in (0, 1)] and None)
        pick((g > 0) & (g <= groups), lambda: cache_load(2, g - 1).start())
        for i, load in enumerate([loads[7], *expert_loads, loads[8]]):
            pick(g == groups + i, load.start)

    start_stage(0)
    loads[0].wait()
    loads[1].wait()
    start_stage(1)
    wide = tokens[...].astype(f32)
    normed = (
        wide * lax.rsqrt(jnp.mean(wide * wide, axis=-1, keepdims=True) + epsilon) * gain[...]
    ).astype(bf16)
    for c in loads[2:4]:
        c.wait()
    pltpu.make_async_copy(wkv, wkv, pair_sem.at[0]).wait()
    start_stage(2)
    start_stage(3)
    query = jnp.dot(normed, wq[...], preferred_element_type=f32).astype(bf16).astype(f32)
    query = query * hd ** (-0.5)
    if beside:
        fresh_pair = jnp.dot(normed, wkv[...], preferred_element_type=f32)
        fresh_pair = fresh_pair[:, :lanes], fresh_pair[:, lanes:]
    else:
        fresh_pair = [jnp.dot(normed, wkv[i], preferred_element_type=f32) for i in range(2)]
    fresh_key, fresh_value = [a.astype(bf16).astype(f32) for a in fresh_pair]
    fresh_values[...] = fresh_value
    fresh_keys[...] = fresh_key
    forget_all = lax.dot_general(
        normed, wf[...], (((1,), (1,)), ((), ())), preferred_element_type=f32
    )
    forget = forget_all[:, 0:heads]
    for j in range(1, tp_count):
        forget = jnp.where(tp == j, forget_all[:, j * heads : (j + 1) * heads], forget)
    forget = jnp.minimum(forget, 0.0) - jnp.log1p(jnp.exp(-jnp.abs(forget)))
    lane_of = lax.broadcasted_iota(jnp.int32, (seqs, lanes), 1) // hd
    for h in range(heads):
        m, place, want = h // per_lane, h % per_lane, h // group_heads
        block = query[:, m * lanes : (m + 1) * lanes]
        if place != want:
            block = pltpu.roll(block, ((want - place) % per_lane) * hd, 1)
        block = jnp.where(lane_of == want, block, 0.0)
        at = pl.ds(h, seqs, stride=heads)
        query_rows[at, :] = block
        forget_rows[at, :] = jnp.broadcast_to(forget[:, h : h + 1], (seqs, lanes))

    position = lax.broadcasted_iota(jnp.int32, (heads, span), 1)

    def rows_at(b):
        return pl.ds(pl.multiple_of(b * heads, heads), heads)

    def score(g):
        for i in range(GROUP):
            b = g * GROUP + i
            scores[g % 2, i] = jnp.dot(
                query_rows[rows_at(b), :].astype(bf16), keys[b], preferred_element_type=f32
            )

    def soften(g):
        for i in range(GROUP):
            b = g * GROUP + i
            length = lengths[b]
            gate = gates[b]
            latest = jnp.sum(
                jnp.where(position == length - 1, gate, 0.0), axis=-1, keepdims=True
            )
            fresh = jnp.sum(
                query_rows[rows_at(b), :] * fresh_keys[pl.ds(b, 1), :], axis=-1, keepdims=True
            )
            past = scores[g % 2, i] + (latest + forget_rows[rows_at(b), :][:, 0:1]) - gate
            past = jnp.where(position < length, past, -jnp.inf)
            peak = jnp.maximum(jnp.max(past, axis=-1, keepdims=True), fresh)
            past = jnp.exp(past - peak)
            fresh = jnp.exp(fresh - peak)
            total = jnp.sum(past, axis=-1, keepdims=True) + fresh
            probs[g % 2, i] = past.astype(bf16)
            fresh_rows[g % 2, i] = jnp.broadcast_to(fresh, (heads, lanes))
            total_rows[g % 2, i] = jnp.broadcast_to(total, (heads, lanes))

    def blend(g):
        for i in range(GROUP):
            b = g * GROUP + i
            mixed = lax.dot_general(
                probs[g % 2, i],
                values[b],
                (((1,), (1,)), ((), ())),
                preferred_element_type=f32,
            )
            mixed_rows[rows_at(b), :] = (
                mixed + fresh_rows[g % 2, i] * fresh_values[pl.ds(b, 1), :]
            ) / total_rows[g % 2, i]

    def arrived(kinds, g):
        for kind in kinds:
            cache_load(kind, g).wait()

    def attend(g, c):
        arrived((0, 1), g)
        arrived((2,), g - 2)
        start_stage(g + AHEAD)
        blend(g - 2)
        soften(g - 1)
        score(g)
        return c

    arrived((0, 1), 0)
    start_stage(AHEAD)
    score(0)
    arrived((0, 1), 1)
    start_stage(AHEAD + 1)
    soften(0)
    score(1)
    lax.fori_loop(2, groups, attend, 0)
    for g in range(groups + AHEAD, groups + 4):
        start_stage(g)
    arrived((2,), groups - 2)
    blend(groups - 2)
    soften(groups - 1)
    arrived((2,), groups - 1)
    blend(groups - 1)

    pieces = []
    for m in range(heads // per_lane):
        piece = jnp.zeros((seqs, lanes), f32)
        for place in range(per_lane):
            h = m * per_lane + place
            want = h // group_heads
            block = mixed_rows[pl.ds(h, seqs, stride=heads), :]
            if place != want:
                block = pltpu.roll(block, ((place - want) % per_lane) * hd, 1)
            piece = jnp.where(lane_of == place, block, piece)
        pieces.append(piece.astype(bf16))
    attended = jnp.concatenate(pieces, axis=1)

    loads[7].wait()
    pl.semaphore_wait(barrier, ep_count - 1 + tp_count - 1)

    def project(peer):
        at = pl.ds(pl.multiple_of(peer * own, own), own)
        part_send[peer] = jnp.dot(
            attended, wo[:, at], preferred_element_type=f32
        ).astype(bf16)

    def received(ref, sem):
        pltpu.make_async_copy(ref, ref, sem).wait()

    def part_copy(peer):
        o = (peer + tp_count - tp) % tp_count
        return pltpu.make_async_remote_copy(
            src_ref=part_send.at[peer],
            dst_ref=part_recv.at[o - 1],
            send_sem=part_ss.at[0],
            recv_sem=part_rs.at[0],
            device_id={"tp": peer},
            device_id_type=MESH,
        )

    for d in [*range(1, chips), 0]:
        for base in (tp, partner):
            if d or base is partner:
                peer = (base + 2 * d) % tp_count
                project(peer)
                part_copy(peer).start()
    project(tp)
    for c in loads[4:7]:
        c.wait()
    slot = lax.broadcasted_iota(jnp.int32, (slots, seqs), 0)
    slot_expert, slot_rank = slot // cap, slot % cap
    first = routes[0:1, :] == slot_expert
    second = routes[1:2, :] == slot_expert
    named = jnp.where(jnp.logical_or(first, second), 1.0, 0.0)
    earlier = jnp.where(
        lax.broadcasted_iota(jnp.int32, (seqs, seqs), 0)
        < lax.broadcasted_iota(jnp.int32, (seqs, seqs), 1),
        1.0,
        0.0,
    )
    rank = jnp.dot(named.astype(bf16), earlier.astype(bf16), preferred_element_type=f32)
    chosen = jnp.where(rank == slot_rank.astype(f32), named, 0.0)
    dispatch = chosen.astype(bf16)
    one, two = logits[0:1, :], logits[1:2, :]
    top = jnp.maximum(one, two)
    e_one, e_two = jnp.exp(one - top), jnp.exp(two - top)
    share = jnp.where(first, e_one / (e_one + e_two), e_two / (e_one + e_two))
    weight = (share * chosen).T
    weight_high = weight.astype(bf16)
    weight_low = (weight - weight_high.astype(f32)).astype(bf16)
    weight_both = jnp.concatenate([weight_high, weight_low], axis=0)

    columns = pl.ds(pl.multiple_of(tp * own, own), own)
    total = part_send[tp].astype(f32)
    received(part_recv, part_rs.at[0])
    for k in range(tp_count - 1):
        total = total + part_recv[k].astype(f32)
    residual = tokens[:, columns].astype(f32) + total

    packed = jnp.dot(dispatch, residual.astype(bf16), preferred_element_type=f32)
    for e in range(ep_count):
        pack_send[e] = packed[e * cap : (e + 1) * cap].astype(bf16)

    paired = ep_count & (ep_count - 1) == 0

    def across(k):
        if not paired:
            return (ep + k) % ep_count
        e, bit = 0, 1
        while bit < ep_count:
            e, bit = e + (ep // bit + k // bit) % 2 * bit, 2 * bit
        return e

    def source(k):
        return across(k) if paired else (ep + ep_count - k) % ep_count

    def pack_copy(k):
        return pltpu.make_async_remote_copy(
            src_ref=pack_send.at[across(k)],
            dst_ref=gathered.at[tp, ep],
            send_sem=pack_ss.at[0],
            recv_sem=pack_rs.at[k],
            device_id={"ep": across(k)},
            device_id_type=MESH,
        )

    def from_chip(base, d):
        return (base + tp_count - 2 * d) % tp_count

    def fan_copy(way, s):
        relayed = way - (chips - 1) if way >= chips else 0
        block = from_chip(tp, relayed) if relayed else tp
        return pltpu.make_async_remote_copy(
            src_ref=gathered.at[block, s],
            dst_ref=gathered.at[block, s],
            send_sem=fan_ss.at[0],
            recv_sem=fan_rs.at[way - 1, s] if 0 < way < chips else fan_all.at[max(0, relayed)],
            device_id={"tp": (tp + 2 * way) % tp_count if 0 < way < chips else partner},
            device_id_type=MESH,
        )

    for k in range(1, ep_count):
        pack_copy(k).start()
    gathered[tp, ep] = pack_send[ep]

    def fan_out(k, c):
        s = source(k)

        @pl.when(k > 0)
        def _():
            pack_copy(k).wait_recv()

        for way in [*range(1, chips), 0]:
            fan_copy(way, s).start()
        return c

    lax.fori_loop(0, ep_count, fan_out, 0)

    def relay(k, c):
        s = source(k)
        for way in range(1, chips):
            fan_copy(way, s).wait_recv()
            fan_copy(chips - 1 + way, s).start()
        return c

    received(wgu, pair_sem.at[1])
    loads[8].wait()

    def rows_of(block):
        rows = jnp.concatenate(
            [gathered[block, s].astype(f32) for s in range(ep_count)], axis=0
        )
        at = pl.ds(pl.multiple_of(block * own, own), own)
        scaled = (rows * post[:, at]).astype(bf16)
        squares = jnp.sum(rows * rows, axis=-1, keepdims=True)
        if joined:
            both = jnp.dot(scaled, wgu[at, :], preferred_element_type=f32)
            return squares, both[:, :inner], both[:, inner:]
        return squares, *[
            jnp.dot(scaled, wgu[i, at, :], preferred_element_type=f32) for i in range(2)
        ]

    def arrive(relayed):
        received(gathered.at[0], fan_all.at[relayed])

    def add(a, b):
        return tuple(x + y for x, y in zip(a, b))

    sums = rows_of(tp)
    lax.fori_loop(0, ep_count, relay, 0)
    arrive(0)
    sums = add(sums, rows_of(partner))
    for d in range(1, chips):
        sums = add(sums, rows_of(from_chip(tp, d)))
    for d in range(1, chips):
        arrive(d)
        sums = add(sums, rows_of(from_chip(partner, d)))
    squares, gate_act, upper = sums
    scale = lax.rsqrt(squares / width + epsilon)
    gate_act = gate_act * scale
    hidden = (gate_act / (1.0 + jnp.exp(-gate_act)) * (upper * scale)).astype(bf16)

    def down(block):
        at = pl.ds(pl.multiple_of(block * own, own), own)
        return jnp.dot(hidden, wd[:, at], preferred_element_type=f32)

    def down_copy(k, e):
        return pltpu.make_async_remote_copy(
            src_ref=down_send.at[k, e],
            dst_ref=down_recv.at[k, e],
            send_sem=down_ss.at[0],
            recv_sem=down_rs.at[k, e] if k < chips - 1 else down_all.at[e],
            device_id={
                "tp": (tp + 2 * (k - chips + 1)) % tp_count if k >= chips else partner
            },
            device_id_type=MESH,
        )

    def turn(k):
        return across(ep_count - 1 - k)

    def spread(ref, rows):
        for e in range(ep_count):
            ref[e] = rows[e * cap : (e + 1) * cap].astype(ref.dtype)

    def start_down(way):
        def one(k, c):
            down_copy(way, turn(k)).start()
            return c

        lax.fori_loop(0, ep_count, one, 0)

    def ret_copy(k):
        return pltpu.make_async_remote_copy(
            src_ref=ret_send.at[across(k)],
            dst_ref=ret_recv.at[ep],
            send_sem=ret_ss.at[0],
            recv_sem=ret_rs.at[0],
            device_id={"ep": across(k)},
            device_id_type=MESH,
        )

    for d in range(1, chips):
        spread(down_send.at[d - 1], down((partner + 2 * d) % tp_count))
        start_down(d - 1)
    for d in range(1, chips):
        spread(held, down((tp + 2 * d) % tp_count))

        def cross(k, c):
            e = turn(k)
            down_copy(d - 1, e).wait_recv()
            down_send[chips - 1 + d, e] = (
                held[e] + down_recv[d - 1, e].astype(f32)
            ).astype(bf16)
            down_copy(chips - 1 + d, e).start()
            return c

        lax.fori_loop(0, ep_count, cross, 0)
    spread(down_send.at[chips - 1], down(partner))
    start_down(chips - 1)
    spread(held, down(tp))

    def give_back(k, c):
        e = turn(k)
        total = held[e]
        received(down_recv.at[pl.ds(chips - 1, chips), e], down_all.at[e])
        for way in range(chips - 1, 2 * chips - 1):
            total = total + down_recv[way, e].astype(f32)

        @pl.when(k < ep_count - 1)
        def _():
            ret_send[e] = total.astype(bf16)
            ret_copy(ep_count - 1 - k).start()

        @pl.when(k == ep_count - 1)
        def _():
            ret_recv[e] = total.astype(bf16)

        return c

    lax.fori_loop(0, ep_count, give_back, 0)

    received(ret_recv.at[pl.ds(0, ep_count - 1)], ret_rs.at[0])
    returned = jnp.concatenate(
        [ret_recv[e].astype(f32) for e in range(ep_count)], axis=0
    ).astype(bf16)
    mix = jnp.dot(weight_both, returned, preferred_element_type=f32)
    out[...] = (residual + (mix[:seqs] + mix[seqs:])).astype(bf16)

    received(part_recv, part_ss.at[0])
    received(ret_recv.at[pl.ds(0, ep_count - 1)], pack_ss.at[0])
    received(ret_recv.at[pl.ds(0, ep_count - 1)], ret_ss.at[0])
    received(down_recv, fan_ss.at[0])
    received(down_recv, down_ss.at[0])


def body(
    tokens,
    norm_gain,
    post_gain,
    w_query,
    w_key,
    w_value,
    w_forget,
    w_output,
    key_cache,
    value_cache,
    gate_cache,
    lengths,
    routes,
    route_logits,
    w_gate,
    w_up,
    w_down,
):
    ep_count = lax.axis_size("ep")
    tp_count = lax.axis_size("tp")
    ways = tp_count - 1
    seqs, width = tokens.shape
    heads, span = gate_cache.shape[1:]
    own = width // tp_count
    cap = 2 * seqs * routes.shape[1] // ep_count
    lanes = key_cache.shape[1] * key_cache.shape[2]
    hbm = [
        tokens,
        norm_gain.reshape(1, width),
        post_gain.reshape(1, width),
        w_query,
        w_key,
        w_value,
        w_forget.T,
        w_output,
        key_cache.reshape(seqs, lanes, span),
        value_cache.reshape(seqs, lanes, span),
        gate_cache,
        routes.T,
        route_logits.T,
        w_gate.reshape(w_gate.shape[1:]),
        w_up.reshape(w_up.shape[1:]),
        w_down.reshape(w_down.shape[1:]),
    ]
    dma = pltpu.SemaphoreType.DMA
    def beside(a):
        rows, columns = a.shape
        return (rows, 2 * columns) if columns % 128 == 0 else (2, rows, columns)

    gate_up = hbm[13:15]
    scratch = [
        pltpu.VMEM(beside(a) if a is w_key or a is gate_up[0] else a.shape, a.dtype)
        for a in hbm
        if a is not w_value and a is not gate_up[1]
    ] + [
        pltpu.VMEM((seqs * heads, lanes), f32),
        pltpu.VMEM((seqs * heads, lanes), f32),
        pltpu.VMEM((seqs, lanes), f32),
        pltpu.VMEM((seqs, lanes), f32),
        pltpu.VMEM((seqs * heads, lanes), f32),
        pltpu.VMEM((2, GROUP, heads, span), f32),
        pltpu.VMEM((2, GROUP, heads, span), bf16),
        pltpu.VMEM((2, GROUP, heads, lanes), f32),
        pltpu.VMEM((2, GROUP, heads, lanes), f32),
        pltpu.VMEM((tp_count, seqs, own), bf16),
        pltpu.VMEM((ways, seqs, own), bf16),
        pltpu.VMEM((ep_count, cap, own), bf16),
        pltpu.VMEM((tp_count, ep_count, cap, own), bf16),
        pltpu.VMEM((ways, ep_count, cap, own), bf16),
        pltpu.VMEM((ways, ep_count, cap, own), bf16),
        pltpu.VMEM((ep_count, cap, own), bf16),
        pltpu.VMEM((ep_count, cap, own), bf16),
        pltpu.VMEM((ep_count, cap, own), f32),
        dma((9,)),
        dma((2,)),
        dma((3, seqs // GROUP)),
        dma((1,)),
        dma((1,)),
        dma((1,)),
        dma((ep_count,)),
        dma((1,)),
        dma((tp_count // 2 - 1, ep_count)),
        dma((tp_count // 2,)),
        dma((1,)),
        dma((tp_count // 2 - 1, ep_count)),
        dma((ep_count,)),
        dma((1,)),
        dma((1,)),
    ]
    return pl.pallas_call(
        functools.partial(layer_kernel, ep_count, tp_count),
        out_shape=pltpu.VMEM((seqs, own), bf16),
        in_specs=[pl.BlockSpec(memory_space=pltpu.SMEM)]
        + [pl.BlockSpec(memory_space=pl.ANY)] * len(hbm),
        out_specs=pl.BlockSpec(memory_space=pltpu.VMEM),
        scratch_shapes=scratch,
        compiler_params=pltpu.CompilerParams(
            collective_id=0, has_side_effects=True, vmem_limit_bytes=48 * 1024 * 1024
        ),
    )(*[pltpu.with_memory_space_constraint(a, pltpu.HBM) for a in [lengths, *hbm]])


def solution(mesh):
    in_specs = (
        P("ep", None),
        P(),
        P(),
        P(None, "tp"),
        P(None, "tp"),
        P(None, "tp"),
        P(),
        P("tp", None),
        P("ep", "tp", None, None),
        P("ep", "tp", None, None),
        P("ep", "tp", None),
        P("ep"),
        P("ep", None),
        P("ep", None),
        P("ep", None, "tp"),
        P("ep", None, "tp"),
        P("ep", "tp", None),
    )
    out_specs = P("ep", "tp")
    return jax.shard_map(body, mesh=mesh, in_specs=in_specs, out_specs=out_specs, check_vma=False)
```
